32 devices in a mesh: sp: 8 (over z, y), tp: 4 (over x, core).
Axes of the slice: x: 2, y: 2, z: 4, core: 2. Of those that a mesh axis runs over, the one named last changes fastest.
Arguments:
- queries: bfloat16 [8192, 1024], P('sp', 'tp'), may hold values from -300 to 300
- keys: bfloat16 [8192, 512], P('sp', 'tp'), may hold values from -6 to 6
- values: bfloat16 [8192, 512], P('sp', 'tp'), may hold values from -6 to 6
- sink_logits: float32 [16], P('tp'), may hold values from 1 to 6
- residual: bfloat16 [8192, 2048], P('sp'), may hold values from -3 to 3
- out_weight: bfloat16 [1024, 2048], P('tp'), may hold values from -0.5390625 to 0.5390625
- norm_gain: float32 [2048], replicated, may hold values from 0.1 to 1.9
- gate_weight: bfloat16 [2048, 5632], P('sp', 'tp'), may hold values from -0.125 to 0.125
- up_weight: bfloat16 [2048, 5632], P('sp', 'tp'), may hold values from -0.125 to 0.125
- down_weight: bfloat16 [2048, 5632], P('sp', 'tp'), may hold values from -0.1796875 to 0.1796875
Outputs:
- layer_out: bfloat16 [8192, 2048], P(('sp', 'tp'))
The draws below stay inside these ranges and needn't reach their ends.
All inputs are finite; a program needn't handle non-finite values.
Results may differ from the reference program's by a relative error of at most 0.02.
Values may be sent and summed in bfloat16 or wider, within the bound.
No kernel may reach another device: no remote copies, remote signals or barrier semaphores. Data moves between devices by JAX's collectives and lax.ppermute only.
A program may use at most 64 MiB of HBM per device.

```python
import jax
import jax.numpy as jnp
from jax import lax

D = 2048
QH = 16
KVH = 8
HD = 64
FF = 5632
WINDOW = 128
TOKENS = 8192
GROUPS = 4


def shared_keys(key):
    base = jax.random.normal(jax.random.fold_in(key, 7), (TOKENS, KVH * HD), jnp.float32)
    base = jnp.clip(base, -6.0, 6.0)
    return base


def draw_keys(key, part):
    return shared_keys(key).astype(jnp.bfloat16)


def draw_queries(key, part):
    drawn = jax.random.normal(jax.random.fold_in(key, 13), (TOKENS, QH * HD), jnp.float32)
    drawn = jnp.clip(drawn, -6.0, 6.0)
    return drawn.astype(jnp.bfloat16)


def steps_of(own_key, extent, split, least, high):
    factor_of = 1.0
    for position, blocks in split:
        steps = jax.random.uniform(jax.random.fold_in(jax.random.fold_in(own_key, 6), position), (blocks,), jnp.float32, least / len(split), high / len(split))
        factor_of = factor_of * jnp.repeat(jnp.exp(steps), extent[position] // blocks).reshape((-1,) + (1,) * (len(extent) - 1 - position))
    return factor_of


def noise(rng, dims, scale, reach, cuts=(), kind=jnp.bfloat16):
    values = scale * jax.random.normal(rng, dims, jnp.float32)
    if cuts:
        values = values * steps_of(rng, dims, cuts, -0.22, 0.18)
    return jnp.clip(values, -reach, reach).astype(kind)


def setup_inputs(seed: int = 0) -> dict:
    seeds = jax.random.split(jax.random.key(seed), 11)
    queries = draw_queries(jax.random.fold_in(seeds[10], 71), 0)
    keys = draw_keys(jax.random.fold_in(seeds[10], 71), 0)
    values = noise(seeds[2], (TOKENS, KVH * HD), 1.0, 6.0, ((0, 8), (1, 4)))
    sink_logits = jnp.clip(1.0 + 5.0 * jax.random.uniform(seeds[3], (QH,), jnp.float32) ** steps_of(seeds[3], (QH,), ((0, 4),), -0.2, 0.2), 1.0, 6.0)
    residual = noise(seeds[4], (TOKENS, D), 0.5, 3.0, ((0, 8),))
    out_weight = noise(seeds[5], (QH * HD, D), 0.09, 0.5390625, ((0, 4),))
    norm_gain = jnp.clip(1.0 + 0.18 * jax.random.normal(seeds[6], (D,), jnp.float32), 0.1, 1.9)
    gate_weight = noise(seeds[7], (D, FF), D ** -0.5, 0.125, ((0, 8), (1, 4)))
    up_weight = noise(seeds[8], (D, FF), D ** -0.5, 0.125, ((0, 8), (1, 4)))
    down_weight = noise(seeds[9], (D, FF), 0.03, 0.1796875, ((0, 8), (1, 4)))
    return dict(queries=queries, keys=keys, values=values, sink_logits=sink_logits, residual=residual, out_weight=out_weight, norm_gain=norm_gain, gate_weight=gate_weight, up_weight=up_weight, down_weight=down_weight)


def attention_rows(queries, keys, values, sink_logits):
    total = queries.shape[0]
    blocks = total // WINDOW
    groups = QH // KVH
    query_blocks = queries.astype(jnp.float32).reshape(blocks, WINDOW, KVH, groups, HD)

    def banded(source):
        shaped = source.astype(jnp.float32).reshape(blocks, WINDOW, KVH, HD)
        earlier = jnp.concatenate([jnp.zeros_like(shaped[:1]), shaped[:-1]], axis=0)
        return jnp.concatenate([earlier, shaped], axis=1)
    key_band = banded(keys)
    value_band = banded(values)
    query_index = jnp.arange(WINDOW, dtype=jnp.int32)[:, None]
    key_index = jnp.arange(2 * WINDOW, dtype=jnp.int32)[None, :]
    distance = query_index - key_index + WINDOW
    key_place = jnp.arange(blocks, dtype=jnp.int32)[:, None, None] * WINDOW + key_index[None] - WINDOW
    valid = (distance >= 0) & (distance < WINDOW) & (key_place >= 0)
    head_number = jnp.arange(1, QH + 1, dtype=jnp.float32)
    slopes = (2.0 ** (-8.0 * head_number / QH)).reshape(KVH, groups, 1, 1, 1)
    scores = jnp.einsum('nqhgd,nkhd->hgnqk', query_blocks, key_band) * HD ** (-0.5)
    scores = scores - slopes * distance.astype(jnp.float32)
    scores = jnp.where(valid, scores, -jnp.inf)
    sinks = sink_logits.astype(jnp.float32).reshape(KVH, groups, 1, 1, 1)
    top = jnp.maximum(lax.optimization_barrier(jnp.max(scores, axis=-1, keepdims=True)), sinks)
    expd = jnp.exp(scores - top)
    denom = lax.optimization_barrier(jnp.sum(expd, axis=-1, keepdims=True)) + jnp.exp(sinks - top)
    weights = (expd / denom).astype(jnp.bfloat16)
    output = jnp.einsum('hgnqk,nkhd->nqhgd', weights.astype(jnp.float32), value_band)
    return output.reshape(total, QH * HD).astype(jnp.bfloat16)

def rounded(term):
    return lax.optimization_barrier(term.astype(jnp.bfloat16)).astype(jnp.float32)

def reference(queries, keys, values, sink_logits, residual, out_weight, norm_gain, gate_weight, up_weight, down_weight):
    attended = attention_rows(queries, keys, values, sink_logits)
    head_cols = QH * HD // GROUPS
    projected = jnp.zeros((queries.shape[0], D), jnp.float32)
    for group in range(GROUPS):
        term = jnp.dot(attended[:, group * head_cols:(group + 1) * head_cols], out_weight[group * head_cols:(group + 1) * head_cols], preferred_element_type=jnp.float32)
        projected = projected + rounded(term)
    mixed = (residual.astype(jnp.float32) + projected).astype(jnp.bfloat16)
    mixed_f = mixed.astype(jnp.float32)
    scale = lax.rsqrt(lax.optimization_barrier(jnp.mean(mixed_f * mixed_f, axis=-1, keepdims=True)) + 1e-06)
    normed = (mixed_f * scale * norm_gain.astype(jnp.float32)).astype(jnp.bfloat16)
    gate = jnp.dot(normed, gate_weight, preferred_element_type=jnp.float32)
    upper = jnp.dot(normed, up_weight, preferred_element_type=jnp.float32)
    hidden = (jax.nn.silu(gate) * upper).astype(jnp.bfloat16)
    unit_cols = FF // GROUPS
    expanded = jnp.zeros((queries.shape[0], D), jnp.float32)
    for group in range(GROUPS):
        term = lax.dot_general(hidden[:, group * unit_cols:(group + 1) * unit_cols], down_weight[:, group * unit_cols:(group + 1) * unit_cols], (((1,), (1,)), ((), ())), preferred_element_type=jnp.float32)
        expanded = expanded + rounded(term)
    return (mixed_f + 0.5 * expanded).astype(jnp.bfloat16)
```

```python
import jax
import jax.numpy as jnp
from jax import lax
from jax.experimental import pallas as pl
from jax.experimental.pallas import tpu as pltpu
from jax.sharding import PartitionSpec as P

QH = 16
HD = 64
WINDOW = 128


def shifted(block, axis, distance):
    devices = range(lax.axis_size(axis))
    route = [(i - distance, i) for i in devices if i - distance in devices]
    return lax.ppermute(block, axis, route)


def attend(queries, keys, values, sink_logits):
    local_rows = queries.shape[0]
    kv_local = keys.shape[1] // HD
    heads_local = queries.shape[1] // HD
    groups = heads_local // kv_local
    blocks = local_rows // WINDOW
    key_value = jnp.concatenate([keys, values], axis=1)
    previous = shifted(key_value[local_rows - WINDOW :], "sp", 1)
    extended = jnp.concatenate([previous, key_value], axis=0)
    stacked = extended.reshape(blocks + 1, WINDOW, 2 * kv_local * HD)
    band = jnp.concatenate([stacked[:-1], stacked[1:]], axis=1)
    key_band = band[:, :, : kv_local * HD].reshape(blocks, 2 * WINDOW, kv_local, HD)
    value_band = band[:, :, kv_local * HD :].reshape(blocks, 2 * WINDOW, kv_local, HD)
    query_blocks = queries.reshape(blocks, WINDOW, kv_local, groups, HD)
    query_index = jnp.arange(WINDOW, dtype=jnp.int32)[:, None]
    key_index = jnp.arange(2 * WINDOW, dtype=jnp.int32)[None, :]
    distance = query_index - key_index + WINDOW
    offset = lax.axis_index("sp") * local_rows
    key_place = (
        offset
        + jnp.arange(blocks, dtype=jnp.int32)[:, None, None] * WINDOW
        + key_index[None]
        - WINDOW
    )
    valid = (distance >= 0) & (distance < WINDOW) & (key_place >= 0)
    head_number = (
        lax.axis_index("tp") * heads_local + jnp.arange(heads_local, dtype=jnp.int32) + 1
    ).astype(jnp.float32)
    slopes = (2.0 ** (-8.0 * head_number / QH)).reshape(kv_local, groups, 1, 1, 1)
    scores = jnp.einsum(
        "nqhgd,nkhd->hgnqk", query_blocks, key_band, preferred_element_type=jnp.float32
    ) * HD ** (-0.5)
    scores = scores - slopes * distance.astype(jnp.float32)
    scores = jnp.where(valid, scores, -jnp.inf)
    sinks = sink_logits.reshape(kv_local, groups, 1, 1, 1)
    top = jnp.maximum(jnp.max(scores, axis=-1, keepdims=True), sinks)
    expd = jnp.exp(scores - top)
    denom = jnp.sum(expd, axis=-1, keepdims=True) + jnp.exp(sinks - top)
    weights = (expd / denom).astype(jnp.bfloat16)
    output = jnp.einsum(
        "hgnqk,nkhd->nqhgd", weights, value_band, preferred_element_type=jnp.float32
    )
    return output.reshape(local_rows, heads_local * HD).astype(jnp.bfloat16)


def rms_scale(rows, norm_gain):
    rows_f = rows.astype(jnp.float32)
    scale = lax.rsqrt(jnp.mean(rows_f * rows_f, axis=-1, keepdims=True) + 1e-06)
    return (rows_f * scale * norm_gain).astype(jnp.bfloat16)


def pair_route(axis):
    return [(i, i ^ 1) for i in range(lax.axis_size(axis))]


def across_route(axis, step):
    count = lax.axis_size(axis)
    return [(i, (i + 2 * step) % count) for i in range(count)]


def hop(block, axis, step):
    route = across_route(axis, step) if step else pair_route(axis)
    return lax.ppermute(block, axis, route)


def gather_ring(block, lines):
    half = block.shape[0] // 2
    reach = lines // 2
    ahead, behind = [block], [block]
    for _ in range(1, reach):
        ahead.append(hop(ahead[-1], "sp", -1))
        behind.append(hop(behind[-1], "sp", 1))
    front = hop(ahead[-1][:half], "sp", -1)
    back = hop(behind[-1][half:], "sp", 1)
    own = hop(block, "sp", 0)
    ahead_side = [own] + [hop(ahead[k], "sp", 0) for k in range(1, reach)]
    behind_side = [hop(behind[k], "sp", 0) for k in range(1, reach)]
    front_side = hop(front, "sp", 0)
    back_side = hop(ahead_side[-1][half:], "sp", -1)
    same = ahead + [front, back] + behind[:0:-1]
    other = ahead_side + [front_side, back_side] + behind_side[::-1]
    return same, other


def add_up(kept, given, chips, own_rows):
    total = kept.astype(jnp.float32) + hop(given, "tp", 0).astype(jnp.float32)
    pieces = []
    for step in range(1, chips):
        piece = total[step * own_rows : (step + 1) * own_rows].astype(jnp.bfloat16)
        pieces.append(hop(piece, "tp", step))
    return [total[:own_rows]] + pieces


def added(terms):
    total = terms[0]
    for term in terms[1:]:
        total = total + term.astype(jnp.float32)
    return total


def close(mixed, same, other, side, spot, lines, shard):
    rows, width = mixed.shape
    if shard % 128:
        sums = [
            turned(added(terms).reshape(rows, lines, 1, shard), (lines - spot) % lines, 1)
            for terms in (same, other)
        ]
        first = jnp.where(side == 0, sums[0], sums[1])
        second = jnp.where(side == 0, sums[1], sums[0])
        expanded = jnp.concatenate([first, second], axis=2).reshape(rows, width)
        return (mixed.astype(jnp.float32) + 0.5 * expanded).astype(jnp.bfloat16)
    count = len(same)

    def body(where, mixed_ref, *refs):
        out_ref = refs[-1]
        near = added([ref[...] for ref in refs[:count]])
        far = added([ref[...] for ref in refs[count:-1]])
        mine = pl.program_id(0) % 2 == where[0]
        expanded = jnp.where(mine, near, far)
        out_ref[...] = (mixed_ref[...].astype(jnp.float32) + 0.5 * expanded).astype(jnp.bfloat16)

    def source(j, where):
        return 0, (j // 2 + lines - where[1]) % lines

    def place(j, where):
        return 0, j

    spec = pl.BlockSpec((rows, shard), source)
    return pl.pallas_call(
        body,
        grid_spec=pltpu.PrefetchScalarGridSpec(
            num_scalar_prefetch=1,
            grid=(2 * lines,),
            in_specs=[pl.BlockSpec((rows, shard), place)] + [spec] * (2 * count),
            out_specs=pl.BlockSpec((rows, shard), place),
        ),
        out_shape=jax.ShapeDtypeStruct((rows, width), jnp.bfloat16),
    )(jnp.stack([side, spot]).astype(jnp.int32), mixed, *same, *other)


def dot_rows(rows, matrix):
    return jnp.dot(rows, matrix, preferred_element_type=jnp.float32)


def dot_back(rows, matrix):
    return lax.dot_general(
        rows, matrix, (((1,), (1,)), ((), ())), preferred_element_type=jnp.float32
    ).astype(jnp.bfloat16)


def turned(block, start, axis):
    size = block.shape[axis]
    return lax.dynamic_slice_in_dim(jnp.concatenate([block, block], axis), start, size, axis)


def per_device(
    queries,
    keys,
    values,
    sink_logits,
    residual,
    out_weight,
    norm_gain,
    gate_weight,
    up_weight,
    down_weight,
):
    local_rows = queries.shape[0]
    tp_count = lax.axis_size("tp")
    chips = tp_count // 2
    own_rows = local_rows // tp_count
    place = lax.axis_index("tp")
    core = place % 2
    side = lax.axis_index("sp") % 2
    spot = lax.axis_index("sp") // 2
    shard = gate_weight.shape[0]
    lines = lax.axis_size("sp") // 2
    half = lines * shard
    gate_same, gate_other = gather_ring(gate_weight, lines)
    up_same, up_other = gather_ring(up_weight, lines)
    down_same, down_other = gather_ring(down_weight, lines)

    attended = attend(queries, keys, values, sink_logits)
    by_place = turned(attended.reshape(chips, 2, own_rows, attended.shape[1]), place // 2, 0)
    kept_rows = lax.dynamic_index_in_dim(by_place, core, 1, False)
    given_rows = lax.dynamic_index_in_dim(by_place, 1 - core, 1, False)
    flat = (chips * own_rows, attended.shape[1])
    given = dot_rows(given_rows.reshape(flat), out_weight).astype(jnp.bfloat16)
    kept = dot_rows(kept_rows.reshape(flat), out_weight).astype(jnp.bfloat16)
    projected = added(add_up(kept, given, chips, own_rows))
    residual_rows = lax.dynamic_slice_in_dim(residual, place * own_rows, own_rows, 0)
    mixed = (residual_rows.astype(jnp.float32) + projected).astype(jnp.bfloat16)

    normed = turned(rms_scale(mixed, norm_gain).reshape(own_rows, lines, 2, shard), spot, 1)
    normed = jnp.concatenate(
        [
            lax.dynamic_index_in_dim(normed, side, 2, False).reshape(own_rows, half),
            lax.dynamic_index_in_dim(normed, 1 - side, 2, False).reshape(own_rows, half),
        ],
        axis=1,
    )
    pieces = [normed] + [hop(normed, "tp", -k) for k in range(1, chips)]
    near = jnp.concatenate(pieces, axis=0)
    rows = jnp.concatenate([near, hop(near, "tp", 0)], axis=0)
    gates, uppers = [], []
    for name, blocks, into in (
        ("gate_one", gate_same, gates),
        ("up_one", up_same, uppers),
        ("gate_two", gate_other, gates),
    ):
        source = rows[:, half:] if name == "gate_two" else rows[:, :half]
        into.append(dot_rows(source, jnp.concatenate(blocks, axis=0)))
    uppers.append(dot_rows(rows[:, half:], jnp.concatenate(up_other, axis=0)))
    gate = gates[0] + gates[1]
    upper = uppers[0] + uppers[1]
    hidden = (jax.nn.silu(gate) * upper).astype(jnp.bfloat16)
    split = chips * own_rows
    sums = []
    for blocks in (down_same, down_other):
        matrix = jnp.concatenate(blocks, axis=0)
        given = dot_back(hidden[split:], matrix)
        kept = dot_back(hidden[:split], matrix)
        sums.append(add_up(kept, given, chips, own_rows))
    return close(mixed, sums[0], sums[1], side, spot, lines, shard)


def solution(mesh):
    return jax.shard_map(
        per_device,
        mesh=mesh,
        in_specs=(
            P("sp", "tp"),
            P("sp", "tp"),
            P("sp", "tp"),
            P("tp"),
            P("sp", None),
            P("tp", None),
            P(),
            P("sp", "tp"),
            P("sp", "tp"),
            P("sp", "tp"),
        ),
        out_specs=P(("sp", "tp"), None),
        check_vma=False,
    )
```
